32 devices in a mesh: grp: 2 (over x), tp: 16 (over z, y, core).
Axes of the slice: x: 2, y: 2, z: 4, core: 2. Of those that a mesh axis runs over, the one named last changes fastest.
Arguments:
- tokens: bfloat16 [96, 4096], P('grp', 'tp'), parts along dimension 0, may hold values from -6 to 6
- states: float32 [2, 96, 32, 128, 128], P(None, 'grp', 'tp'), parts along dimension 1, may hold values from -10 to 10
- norm_gain: float32 [2, 4096], replicated, may hold values from 0.1 to 1.9
- query_weight: bfloat16 [2, 4096, 4096], P(None, None, 'tp'), may hold values from -0.09375 to 0.09375
- forget_weight: bfloat16 [2, 4096, 4096], P(None, None, 'tp'), may hold values from -0.09375 to 0.09375
- value_weight: bfloat16 [2, 4096, 4096], P(None, None, 'tp'), may hold values from -0.09375 to 0.09375
- gate_weight: bfloat16 [2, 4096, 4096], P(None, None, 'tp'), may hold values from -0.09375 to 0.09375
- output_weight: bfloat16 [2, 4096, 4096], P(None, 'tp'), may hold values from -0.125 to 0.125
- output_gain: float32 [2, 4096], P(None, 'tp'), may hold values from 0.1 to 1.9
- bound_logits: float32 [4096], P('tp'), may hold values from -6 to 6
Outputs:
- mixed: bfloat16 [96, 4096], P('grp', 'tp'), parts along dimension 0
- new_states: float32 [2, 96, 32, 128, 128], P(None, 'grp', 'tp'), parts along dimension 1
The draws below stay inside these ranges and needn't reach their ends.
There are 2 independent parts, one for each index of `grp`. The reference program is written for one: setup_inputs(seed, part) draws one part's arguments, and reference() takes and returns one part's arrays. A program takes and returns all parts, laid end to end along the dimension named above; an argument that names none is the same for every part. Nothing has to cross between parts.
All inputs are finite; a program needn't handle non-finite values.
Results may differ from the reference program's by a relative error of at most 0.017.
Values may be sent and summed in bfloat16 or wider, within the bound.
A program may use at most 128 MiB of HBM per device.

```python
import jax
import jax.numpy as jnp
from jax import lax

HEADS = 32
HEAD_DIM = 128
WIDTH = 4096
BATCH = 48


def draw_states(key, part):
    first_key = jax.random.fold_in(jax.random.fold_in(key, 17), 0)
    shape = (2, BATCH, HEADS, HEAD_DIM, HEAD_DIM)
    head_pos = jnp.arange(HEADS, dtype=jnp.float32) / (HEADS - 1)
    rising = 0.4 * jnp.power(6.0, head_pos)
    base = jnp.clip(jax.random.normal(first_key, shape, jnp.float32), -4.0, 4.0)
    return base * rising[None, None, :, None, None]


def with_spikes(entries, stream_key, source, target, parts, factor):
    owner, partner = [(jnp.arange(entries.shape[axis_at]) // (entries.shape[axis_at] // parts)).reshape([-1 if axis == axis_at else 1 for axis in range(entries.ndim)]) for axis_at in (source, target)]
    chosen = jax.random.permutation(stream_key, parts)[partner]
    strong = (owner == chosen) | (owner == (partner + parts // 2) % parts)
    return jnp.where(strong, factor * entries, entries)


def level_of(rng, dims, cuts, smallest, high):
    loudness, own = 1.0, jax.random.fold_in(rng, 6)
    for position, parts in cuts:
        draws = jnp.exp(jax.random.uniform(jax.random.fold_in(own, position), (parts,), jnp.float32, smallest / len(cuts), high / len(cuts)))
        loudness = loudness * jnp.repeat(draws, dims[position] // parts).reshape([-1 if axis == position else 1 for axis in range(len(dims))])
    return loudness


def scatter_about(own_key, extent, scale, reach, shards=(), held_as=jnp.bfloat16):
    result = jax.random.normal(own_key, extent, jnp.float32) * scale
    if len(shards) > 0:
        result = level_of(own_key, extent, shards, -0.22, 0.18) * result
    return jnp.clip(result, min=-reach, max=reach).astype(held_as)


def gaussian_with(key, dims, deviation, most, cuts, heavy, kind=jnp.bfloat16):
    entries = deviation * jax.random.normal(key, dims, jnp.float32)
    if cuts:
        entries = entries * level_of(key, dims, cuts, -0.22, 0.18)
    return jnp.clip(with_spikes(entries, jax.random.fold_in(key, 3), *heavy), -most, most).astype(kind)


def setup_inputs(seed: int = 0, part: int = 0) -> dict:
    arg_keys = jax.random.split(jax.random.key(seed), 11)
    part_keys = jax.random.split(jax.random.fold_in(arg_keys[10], part), 11)
    tokens = scatter_about(part_keys[0], (BATCH, WIDTH), 1.0, 6.0, ((1, 16),))
    states = draw_states(jax.random.fold_in(jax.random.fold_in(arg_keys[10], part), 71), part)
    norm_gain = jnp.clip(1.0 + 0.18 * jax.random.normal(arg_keys[2], (2, WIDTH), jnp.float32), 0.1, 1.9)
    query_weight = scatter_about(arg_keys[3], (2, WIDTH, WIDTH), WIDTH ** -0.5, 0.09375, ((2, 16),))
    forget_weight = scatter_about(arg_keys[4], (2, WIDTH, WIDTH), WIDTH ** -0.5, 0.09375, ((2, 16),))
    value_weight = scatter_about(arg_keys[5], (2, WIDTH, WIDTH), WIDTH ** -0.5, 0.09375, ((2, 16),))
    gate_weight = scatter_about(arg_keys[6], (2, WIDTH, WIDTH), WIDTH ** -0.5, 0.09375, ((2, 16),))
    output_weight = gaussian_with(arg_keys[7], (2, WIDTH, WIDTH), WIDTH ** -0.5, 0.125, ((1, 16),), (1, 2, 16, 2.0))
    output_gain = jnp.clip(1.0 + 0.18 * jax.random.normal(arg_keys[8], (2, WIDTH), jnp.float32), 0.1, 1.9)
    bound_logits = scatter_about(arg_keys[9], (WIDTH,), 1.5, 6.0, ((0, 16),), jnp.float32)
    return {"tokens": tokens, "states": states, "norm_gain": norm_gain, "query_weight": query_weight, "forget_weight": forget_weight, "value_weight": value_weight, "gate_weight": gate_weight, "output_weight": output_weight, "output_gain": output_gain, "bound_logits": bound_logits}


epsilon = 1e-06

def mixer_block(stream, state_in, gain_in, query_mat, forget_mat, value_mat, gate_mat, out_mat, gain_out, lower_bound):
    stream32 = stream.astype(jnp.float32)
    factor = lax.rsqrt(lax.optimization_barrier(jnp.mean(stream32 * stream32, axis=-1, keepdims=True)) + epsilon)
    normed = (stream32 * factor * gain_in).astype(jnp.bfloat16)
    query_proj = jnp.dot(normed, query_mat, preferred_element_type=jnp.float32).astype(jnp.bfloat16)
    forget_pre = jnp.dot(normed, forget_mat, preferred_element_type=jnp.float32).astype(jnp.bfloat16)
    value_proj = jnp.dot(normed, value_mat, preferred_element_type=jnp.float32).astype(jnp.bfloat16)
    gate_proj = jnp.dot(normed, gate_mat, preferred_element_type=jnp.float32).astype(jnp.bfloat16)
    forget = lower_bound + (1.0 - lower_bound) * jax.nn.sigmoid(forget_pre.astype(jnp.float32))
    rows = stream.shape[0]
    forget_heads = forget.reshape(rows, HEADS, HEAD_DIM)
    value_heads = value_proj.astype(jnp.float32).reshape(rows, HEADS, HEAD_DIM)
    query_heads = query_proj.astype(jnp.float32).reshape(rows, HEADS, HEAD_DIM) * HEAD_DIM ** (-0.5)
    updated = forget_heads[..., None] * state_in + (1.0 - forget_heads)[..., None] * value_heads[:, :, None, :]
    readout = jnp.einsum('bhk,bhkv->bhv', query_heads, updated, precision=lax.Precision.HIGHEST).reshape(rows, WIDTH)
    energy = lax.optimization_barrier(jnp.sum(readout * readout, axis=-1, keepdims=True))
    gated_rows = (readout * gain_out * jax.nn.silu(gate_proj.astype(jnp.float32))).astype(jnp.bfloat16)
    branch = jnp.dot(gated_rows, out_mat, preferred_element_type=jnp.float32) * lax.rsqrt(energy / WIDTH + epsilon)
    return ((stream32 + branch).astype(jnp.bfloat16), updated)

def reference(tokens, states, norm_gain, query_weight, forget_weight, value_weight, gate_weight, output_weight, output_gain, bound_logits):
    first, state_first = mixer_block(tokens, states[0], norm_gain[0], query_weight[0], forget_weight[0], value_weight[0], gate_weight[0], output_weight[0], output_gain[0], 0.0)
    mixed, state_second = mixer_block(first, states[1], norm_gain[1], query_weight[1], forget_weight[1], value_weight[1], gate_weight[1], output_weight[1], output_gain[1], jax.nn.sigmoid(bound_logits))
    return (mixed, jnp.stack([state_first, state_second]))
```

```python
import functools

import jax
import jax.numpy as jnp
from jax import lax
from jax.experimental import pallas as pl
from jax.experimental.pallas import tpu as pltpu
from jax.sharding import PartitionSpec as P

epsilon = 1e-06


def kernel(
    n,
    tok,
    states,
    gain,
    wq,
    wf,
    wv,
    wg,
    wo,
    ogain,
    blog,
    mixed,
    new,
    w_s,
    wo_s,
    gain_s,
    ogain_s,
    blog_s,
    xg,
    acc,
    ss,
    tf,
    tq,
    v_s,
    ro_s,
    g_s,
    sb,
    ra,
    pb,
    rb,
    es,
    er,
    ep,
    eb,
    sm_sem,
    w_sem,
    gs,
    gr,
    fs,
    fr,
    asend,
    arecv,
    bsend,
    brecv,
    essend,
    esrecv,
    ebsend,
    ebrecv,
):
    rows, cols = tok.shape
    width = cols * n
    heads = states.shape[2]
    size = states.shape[3]
    groups = rows // 8
    half = n // 2
    me = lax.axis_index("tp")
    sib = me + 1 - 2 * lax.rem(me, 2)

    def peer(s):
        return lax.rem(me + 2 * s, n)

    def origin(s):
        return lax.rem(me - 2 * s + n, n)

    def sib_origin(s):
        return lax.rem(sib - 2 * s + n, n)

    def span(d):
        return pl.ds(pl.multiple_of(d * cols, cols), cols)

    def remote(src, dst, send, recv, d):
        return pltpu.make_async_remote_copy(
            src_ref=src,
            dst_ref=dst,
            send_sem=send,
            recv_sem=recv,
            device_id={"tp": d},
            device_id_type=pl.DeviceIdType.MESH,
        )

    barrier = pltpu.get_barrier_semaphore()

    def greet(d):
        pl.semaphore_signal(
            barrier, inc=1, device_id={"tp": d}, device_id_type=pl.DeviceIdType.MESH
        )

    greet(sib)

    @pl.loop(1, half)
    def _(s):
        greet(peer(s))

    tok_copy = pltpu.make_async_copy(tok, xg.at[0, me], sm_sem.at[0])
    tok_copy.start()
    gain_copy = pltpu.make_async_copy(gain, gain_s, sm_sem.at[1])
    gain_copy.start()
    og_copy = pltpu.make_async_copy(ogain, ogain_s, sm_sem.at[2])
    og_copy.start()
    bl_copy = pltpu.make_async_copy(blog, blog_s, sm_sem.at[3])
    bl_copy.start()

    def weight_copies(l):
        return [
            pltpu.make_async_copy(w.at[l], w_s.at[l, i], w_sem.at[l, i])
            for i, w in enumerate((wq, wf, wv, wg))
        ]

    def later_copies(l):
        return [
            pltpu.make_async_copy(states.at[l], new.at[l], w_sem.at[l, 4]),
            pltpu.make_async_copy(wo.at[l], wo_s.at[l], w_sem.at[l, 5]),
        ]

    for c in weight_copies(0):
        c.start()
    for c in later_copies(0):
        c.start()
    for c in weight_copies(1):
        c.start()
    for c in later_copies(1):
        c.start()
    pl.semaphore_wait(barrier, half)
    tok_copy.wait()

    def gather_copy(l, s):
        return remote(xg.at[l, me], xg.at[l, me], gs.at[l, s], gr.at[l, s], peer(s))

    def forward_copy(l, s):
        o = origin(s)
        return remote(xg.at[l, o], xg.at[l, o], fs.at[l, s], fr.at[l, s], sib)

    def a_copy(l, s):
        return remote(sb.at[l, s], ra.at[l, s], asend.at[l, s], arecv.at[l, s], sib)

    def b_copy(l, s):
        return remote(pb.at[l, s], rb.at[l, s], bsend.at[l, s], brecv.at[l, s], peer(s))

    def es_copy(l):
        return remote(es.at[l], er.at[l], essend.at[l], esrecv.at[l], sib)

    def eb_copy(l, s):
        return remote(ep.at[l], eb.at[l, s], ebsend.at[l, s], ebrecv.at[l, s], peer(s))

    for l in range(2):
        forward_copy(l, 0).start()

        @pl.loop(1, half)
        def _(s):
            gather_copy(l, s).start()

        acc[...] = jnp.zeros_like(acc)
        ss[...] = jnp.zeros_like(ss)

        def chunk(o):
            x = xg[l, o].astype(jnp.float32)
            square = x * x
            total = square[:, :128]
            for c in range(128, cols, 128):
                total = total + square[:, c : c + 128]
            ss[...] += total
            scaled = (x * gain_s[l : l + 1, span(o)]).astype(jnp.bfloat16)
            for i in range(4):
                acc[i] += jnp.dot(
                    scaled, w_s[l, i, span(o), :], preferred_element_type=jnp.float32
                )

        if l == 0:
            gain_copy.wait()
        for c in weight_copies(l):
            c.wait()
        chunk(me)

        @pl.loop(1, half)
        def _(s):
            gather_copy(l, s).wait_recv()
            forward_copy(l, s).start()
            chunk(origin(s))
            forward_copy(l, s - 1).wait_recv()
            chunk(sib_origin(s - 1))

        forward_copy(l, half - 1).wait_recv()
        chunk(sib_origin(half - 1))

        factor = lax.rsqrt(jnp.sum(ss[...], axis=-1, keepdims=True) / width + epsilon)

        def projected(i):
            return (acc[i] * factor).astype(jnp.bfloat16).astype(jnp.float32)

        if l == 0:
            og_copy.wait()
            bl_copy.wait()
        query = projected(0) * size**-0.5
        forget = jax.nn.sigmoid(projected(1))
        if l == 1:
            lower = jax.nn.sigmoid(blog_s[...])
            forget = lower + (1.0 - lower) * forget
        v_s[...] = projected(2)
        pad = jnp.zeros((size - rows, size), jnp.float32)
        for h in range(heads):
            for source, dest in ((forget, tf), (query, tq)):
                part = source[:, h * size : (h + 1) * size]
                flipped = jnp.concatenate([part, pad], axis=0).T
                for b in range(groups):
                    shift = (size - 8 * b) % size
                    dest[b, h] = pltpu.roll(flipped, shift, 1) if shift else flipped
        state_copy, wo_copy = later_copies(l)
        state_copy.wait()

        @pl.loop(0, groups)
        def _(b):
            base = pl.multiple_of(b * 8, 8)
            for h in range(heads):
                lanes = slice(h * size, (h + 1) * size)
                values = v_s[pl.ds(base, 8), lanes]
                lines = []
                for j in range(8):
                    value = values[j : j + 1, :]
                    keep = tf[b, h, :, j : j + 1]
                    ask = tq[b, h, :, j : j + 1]
                    updated = keep * (new[l, base + j, h] - value) + value
                    new[l, base + j, h] = updated
                    lines.append(jnp.sum(ask * updated, axis=0, keepdims=True))
                ro_s[pl.ds(base, 8), lanes] = jnp.concatenate(lines, axis=0)

        readout = ro_s[...]
        energy = jnp.sum(readout * readout, axis=-1, keepdims=True)
        lane = lax.broadcasted_iota(jnp.int32, (8, 128), 1)
        tile = jnp.zeros((8, 128), jnp.float32)
        for b in range(groups):
            tile = jnp.where(lane == b, energy[8 * b : 8 * b + 8], tile)
        es[l] = tile
        g_s[...] = (readout * ogain_s[l : l + 1, :] * jax.nn.silu(projected(3))).astype(
            jnp.bfloat16
        )
        es_copy(l).start()
        wo_copy.wait()

        def product(d):
            return jnp.dot(
                g_s[...], wo_s[l, :, span(d)], preferred_element_type=jnp.float32
            )

        @pl.loop(0, half)
        def _(t):
            s = lax.rem(t + 1, half)
            sb[l, s] = product(lax.rem(sib + 2 * s, n)).astype(jnp.bfloat16)
            a_copy(l, s).start()

        es_copy(l).wait_recv()
        ep[l] = es[l] + er[l]

        @pl.loop(1, half)
        def _(s):
            eb_copy(l, s).start()
            mine = product(peer(s))
            a_copy(l, s).wait_recv()
            pb[l, s] = (mine + ra[l, s].astype(jnp.float32)).astype(jnp.bfloat16)
            b_copy(l, s).start()

        mine = product(me)
        a_copy(l, 0).wait_recv()
        mine = mine + ra[l, 0].astype(jnp.float32)

        def collect(s, carry):
            total, powers = carry
            eb_copy(l, s).wait_recv()
            b_copy(l, s).wait_recv()
            return total + rb[l, s].astype(jnp.float32), powers + eb[l, s]

        total, powers = lax.fori_loop(1, half, collect, (mine, ep[l]))
        column = jnp.concatenate([powers[:, b : b + 1] for b in range(groups)], axis=0)
        rescale = lax.rsqrt(column / width + epsilon)
        stream = (xg[l, me].astype(jnp.float32) + total * rescale).astype(jnp.bfloat16)
        if l == 0:
            xg[1, me] = stream
        else:
            mixed[...] = stream

    for l in range(2):
        forward_copy(l, 0).wait_send()
        a_copy(l, 0).wait_send()
        es_copy(l).wait_send()

        @pl.loop(1, half)
        def _(s):
            gather_copy(l, s).wait_send()
            forward_copy(l, s).wait_send()
            a_copy(l, s).wait_send()
            b_copy(l, s).wait_send()
            eb_copy(l, s).wait_send()


def body(
    n,
    tokens,
    states,
    norm_gain,
    query_weight,
    forget_weight,
    value_weight,
    gate_weight,
    output_weight,
    output_gain,
    bound_logits,
):
    rows, cols = tokens.shape
    width = cols * n
    heads, size = states.shape[2:4]
    groups = rows // 8
    half = n // 2
    f32, b16 = jnp.float32, jnp.bfloat16
    dma = pltpu.SemaphoreType.DMA
    anywhere = pl.BlockSpec(memory_space=pl.ANY)
    in_vmem = pl.BlockSpec(memory_space=pltpu.VMEM)
    mixed, new = pl.pallas_call(
        functools.partial(kernel, n),
        out_shape=(
            jax.ShapeDtypeStruct(tokens.shape, b16),
            pltpu.VMEM(states.shape, f32),
        ),
        in_specs=[anywhere] * 10,
        out_specs=(in_vmem, in_vmem),
        scratch_shapes=[
            pltpu.VMEM((2, 4, width, cols), b16),
            pltpu.VMEM((2, cols, width), b16),
            pltpu.VMEM((2, width), f32),
            pltpu.VMEM((2, cols), f32),
            pltpu.VMEM((1, cols), f32),
            pltpu.VMEM((2, n, rows, cols), b16),
            pltpu.VMEM((4, rows, cols), f32),
            pltpu.VMEM((rows, 128), f32),
            pltpu.VMEM((groups, heads, size, size), f32),
            pltpu.VMEM((groups, heads, size, size), f32),
            pltpu.VMEM((rows, cols), f32),
            pltpu.VMEM((rows, cols), f32),
            pltpu.VMEM((rows, cols), b16),
            pltpu.VMEM((2, half, rows, cols), b16),
            pltpu.VMEM((2, half, rows, cols), b16),
            pltpu.VMEM((2, half, rows, cols), b16),
            pltpu.VMEM((2, half, rows, cols), b16),
            pltpu.VMEM((2, 8, 128), f32),
            pltpu.VMEM((2, 8, 128), f32),
            pltpu.VMEM((2, 8, 128), f32),
            pltpu.VMEM((2, half, 8, 128), f32),
            dma((4,)),
            dma((2, 6)),
            dma((2, half)),
            dma((2, half)),
            dma((2, half)),
            dma((2, half)),
            dma((2, half)),
            dma((2, half)),
            dma((2, half)),
            dma((2, half)),
            dma((2,)),
            dma((2,)),
            dma((2, half)),
            dma((2, half)),
        ],
        compiler_params=pltpu.CompilerParams(
            collective_id=0, has_side_effects=True, vmem_limit_bytes=46000 * 1024
        ),
    )(
        tokens,
        states,
        norm_gain,
        query_weight,
        forget_weight,
        value_weight,
        gate_weight,
        output_weight,
        output_gain,
        bound_logits.reshape(1, cols),
    )
    return mixed, new


def solution(mesh):
    placed = (
        P("grp", "tp"),
        P(None, "grp", "tp", None, None),
        P(),
        P(None, None, "tp"),
        P(None, None, "tp"),
        P(None, None, "tp"),
        P(None, None, "tp"),
        P(None, "tp", None),
        P(None, "tp"),
        P("tp"),
    )
    return jax.shard_map(
        functools.partial(body, mesh.shape["tp"]),
        mesh=mesh,
        in_specs=placed,
        out_specs=(P("grp", "tp"), P(None, "grp", "tp", None, None)),
        check_vma=False,
    )
```

```python
import functools

import jax
import jax.numpy as jnp
from jax import lax
from jax.experimental import pallas as pl
from jax.experimental.pallas import tpu as pltpu
from jax.sharding import PartitionSpec as P

epsilon = 1e-06


def kernel(
    n,
    tok,
    states,
    gain,
    wq,
    wf,
    wv,
    wg,
    wo,
    ogain,
    blog,
    mixed,
    new,
    w_s,
    wo_s,
    gain_s,
    ogain_s,
    blog_s,
    xg,
    acc,
    ss,
    tf,
    tq,
    v_s,
    ro_s,
    g_s,
    sb,
    ra,
    pb,
    rb,
    es,
    er,
    ep,
    eb,
    sm_sem,
    w_sem,
    gs,
    gr,
    fs,
    fr,
    asend,
    arecv,
    bsend,
    brecv,
    essend,
    esrecv,
    ebsend,
    ebrecv,
):
    rows, cols = tok.shape
    width = cols * n
    heads = states.shape[2]
    size = states.shape[3]
    groups = rows // 8
    half = n // 2
    me = lax.axis_index("tp")
    sib = me + 1 - 2 * lax.rem(me, 2)

    def peer(s):
        return lax.rem(me + 2 * s, n)

    def origin(s):
        return lax.rem(me - 2 * s + n, n)

    def sib_origin(s):
        return lax.rem(sib - 2 * s + n, n)

    def span(d):
        return pl.ds(pl.multiple_of(d * cols, cols), cols)

    def remote(src, dst, send, recv, d):
        return pltpu.make_async_remote_copy(
            src_ref=src,
            dst_ref=dst,
            send_sem=send,
            recv_sem=recv,
            device_id={"tp": d},
            device_id_type=pl.DeviceIdType.MESH,
        )

    barrier = pltpu.get_barrier_semaphore()

    def greet(d):
        pl.semaphore_signal(
            barrier, inc=1, device_id={"tp": d}, device_id_type=pl.DeviceIdType.MESH
        )

    greet(sib)

    @pl.loop(1, half)
    def _(s):
        greet(peer(s))

    tok_copy = pltpu.make_async_copy(tok, xg.at[0, me], sm_sem.at[0])
    tok_copy.start()
    gain_copy = pltpu.make_async_copy(gain, gain_s, sm_sem.at[1])
    gain_copy.start()
    og_copy = pltpu.make_async_copy(ogain, ogain_s, sm_sem.at[2])
    og_copy.start()
    bl_copy = pltpu.make_async_copy(blog, blog_s, sm_sem.at[3])
    bl_copy.start()

    def weight_copies(l):
        return [
            pltpu.make_async_copy(w.at[l], w_s.at[l, i], w_sem.at[l, i])
            for i, w in enumerate((wq, wf, wv, wg))
        ]

    def later_copies(l):
        return [
            pltpu.make_async_copy(states.at[l], new.at[l], w_sem.at[l, 4]),
            pltpu.make_async_copy(wo.at[l], wo_s.at[l], w_sem.at[l, 5]),
        ]

    for c in weight_copies(0):
        c.start()
    pl.semaphore_wait(barrier, half)
    tok_copy.wait()

    def gather_copy(l, s):
        return remote(xg.at[l, me], xg.at[l, me], gs.at[l, s], gr.at[l, s], peer(s))

    def forward_copy(l, s):
        o = origin(s)
        return remote(xg.at[l, o], xg.at[l, o], fs.at[l, s], fr.at[l, s], sib)

    def a_copy(l, s):
        return remote(sb.at[l, s], ra.at[l, s], asend.at[l, s], arecv.at[l, s], sib)

    def b_copy(l, s):
        return remote(pb.at[l, s], rb.at[l, s], bsend.at[l, s], brecv.at[l, s], peer(s))

    def es_copy(l):
        return remote(es.at[l], er.at[l], essend.at[l], esrecv.at[l], sib)

    def eb_copy(l, s):
        return remote(ep.at[l], eb.at[l, s], ebsend.at[l, s], ebrecv.at[l, s], peer(s))

    for l in range(2):
        forward_copy(l, 0).start()

        @pl.loop(1, half)
        def _(s):
            gather_copy(l, s).start()

        acc[...] = jnp.zeros_like(acc)
        ss[...] = jnp.zeros_like(ss)

        def chunk(o):
            x = xg[l, o].astype(jnp.float32)
            square = x * x
            total = square[:, :128]
            for c in range(128, cols, 128):
                total = total + square[:, c : c + 128]
            ss[...] += total
            scaled = (x * gain_s[l : l + 1, span(o)]).astype(jnp.bfloat16)
            for i in range(4):
                acc[i] += jnp.dot(
                    scaled, w_s[l, i, span(o), :], preferred_element_type=jnp.float32
                )

        if l == 0:
            gain_copy.wait()
        for c in weight_copies(l):
            c.wait()
        if l == 0:
            for c in later_copies(0):
                c.start()
        chunk(me)
        forward_copy(l, 0).wait_recv()
        chunk(sib_origin(0))

        @pl.loop(1, half)
        def _(s):
            gather_copy(l, s).wait_recv()
            forward_copy(l, s).start()
            chunk(origin(s))

        @pl.loop(1, half)
        def _(s):
            forward_copy(l, s).wait_recv()
            chunk(sib_origin(s))

        factor = lax.rsqrt(jnp.sum(ss[...], axis=-1, keepdims=True) / width + epsilon)

        def projected(i):
            return (acc[i] * factor).astype(jnp.bfloat16).astype(jnp.float32)

        if l == 0:
            og_copy.wait()
            bl_copy.wait()
        query = projected(0) * size**-0.5
        forget = jax.nn.sigmoid(projected(1))
        if l == 1:
            lower = jax.nn.sigmoid(blog_s[...])
            forget = lower + (1.0 - lower) * forget
        value = projected(2)
        v_s[...] = value
        kept = query * forget
        fresh = query - kept
        pad = jnp.zeros((size - rows, size), jnp.float32)

        def flip(source, dest):
            for h in range(heads):
                part = source[:, h * size : (h + 1) * size]
                flipped = jnp.concatenate([part, pad], axis=0).T
                for b in range(groups):
                    shift = (size - 8 * b) % size
                    dest[b, h] = pltpu.roll(flipped, shift, 1) if shift else flipped

        flip(kept, tq)
        state_copy, wo_copy = later_copies(l)
        state_copy.wait()

        @pl.loop(0, groups)
        def _(b):
            base = pl.multiple_of(b * 8, 8)
            for h in range(heads):
                lanes = slice(h * size, (h + 1) * size)
                lines = []
                for j in range(8):
                    ask = tq[b, h, :, j : j + 1]
                    lines.append(
                        jnp.sum(ask * new[l, base + j, h], axis=0, keepdims=True)
                    )
                ro_s[pl.ds(base, 8), lanes] = jnp.concatenate(lines, axis=0)

        for h in range(heads):
            lanes = slice(h * size, (h + 1) * size)
            share = jnp.sum(fresh[:, lanes], axis=-1, keepdims=True)
            ro_s[:, lanes] += share * value[:, lanes]

        readout = ro_s[...]
        energy = jnp.sum(readout * readout, axis=-1, keepdims=True)
        lane = lax.broadcasted_iota(jnp.int32, (8, 128), 1)
        tile = jnp.zeros((8, 128), jnp.float32)
        for b in range(groups):
            tile = jnp.where(lane == b, energy[8 * b : 8 * b + 8], tile)
        es[l] = tile
        g_s[...] = (readout * ogain_s[l : l + 1, :] * jax.nn.silu(projected(3))).astype(
            jnp.bfloat16
        )
        es_copy(l).start()
        wo_copy.wait()
        if l == 0:
            for c in weight_copies(1) + later_copies(1):
                c.start()

        def product(d):
            return jnp.dot(
                g_s[...], wo_s[l, :, span(d)], preferred_element_type=jnp.float32
            )

        @pl.loop(0, half)
        def _(t):
            s = lax.rem(t + 1, half)
            sb[l, s] = product(lax.rem(sib + 2 * s, n)).astype(jnp.bfloat16)
            a_copy(l, s).start()

        es_copy(l).wait_recv()
        ep[l] = es[l] + er[l]

        @pl.loop(1, half)
        def _(s):
            eb_copy(l, s).start()
            mine = product(peer(s))
            a_copy(l, s).wait_recv()
            pb[l, s] = (mine + ra[l, s].astype(jnp.float32)).astype(jnp.bfloat16)
            b_copy(l, s).start()

        mine = product(me)
        a_copy(l, 0).wait_recv()
        mine = mine + ra[l, 0].astype(jnp.float32)

        flip(forget, tf)

        @pl.loop(0, groups)
        def _(b):
            base = pl.multiple_of(b * 8, 8)
            for h in range(heads):
                values = v_s[pl.ds(base, 8), h * size : (h + 1) * size]
                for j in range(8):
                    line = values[j : j + 1, :]
                    keep = tf[b, h, :, j : j + 1]
                    new[l, base + j, h] = keep * (new[l, base + j, h] - line) + line

        def collect(s, carry):
            total, powers = carry
            eb_copy(l, s).wait_recv()
            b_copy(l, s).wait_recv()
            return total + rb[l, s].astype(jnp.float32), powers + eb[l, s]

        total, powers = lax.fori_loop(1, half, collect, (mine, ep[l]))
        column = jnp.concatenate([powers[:, b : b + 1] for b in range(groups)], axis=0)
        rescale = lax.rsqrt(column / width + epsilon)
        stream = (xg[l, me].astype(jnp.float32) + total * rescale).astype(jnp.bfloat16)
        if l == 0:
            xg[1, me] = stream
        else:
            mixed[...] = stream

    for l in range(2):
        forward_copy(l, 0).wait_send()
        a_copy(l, 0).wait_send()
        es_copy(l).wait_send()

        @pl.loop(1, half)
        def _(s):
            gather_copy(l, s).wait_send()
            forward_copy(l, s).wait_send()
            a_copy(l, s).wait_send()
            b_copy(l, s).wait_send()
            eb_copy(l, s).wait_send()


def body(
    n,
    tokens,
    states,
    norm_gain,
    query_weight,
    forget_weight,
    value_weight,
    gate_weight,
    output_weight,
    output_gain,
    bound_logits,
):
    rows, cols = tokens.shape
    width = cols * n
    heads, size = states.shape[2:4]
    groups = rows // 8
    half = n // 2
    f32, b16 = jnp.float32, jnp.bfloat16
    dma = pltpu.SemaphoreType.DMA
    anywhere = pl.BlockSpec(memory_space=pl.ANY)
    in_vmem = pl.BlockSpec(memory_space=pltpu.VMEM)
    mixed, new = pl.pallas_call(
        functools.partial(kernel, n),
        out_shape=(
            jax.ShapeDtypeStruct(tokens.shape, b16),
            pltpu.VMEM(states.shape, f32),
        ),
        in_specs=[anywhere] * 10,
        out_specs=(in_vmem, in_vmem),
        scratch_shapes=[
            pltpu.VMEM((2, 4, width, cols), b16),
            pltpu.VMEM((2, cols, width), b16),
            pltpu.VMEM((2, width), f32),
            pltpu.VMEM((2, cols), f32),
            pltpu.VMEM((1, cols), f32),
            pltpu.VMEM((2, n, rows, cols), b16),
            pltpu.VMEM((4, rows, cols), f32),
            pltpu.VMEM((rows, 128), f32),
            pltpu.VMEM((groups, heads, size, size), f32),
            pltpu.VMEM((groups, heads, size, size), f32),
            pltpu.VMEM((rows, cols), f32),
            pltpu.VMEM((rows, cols), f32),
            pltpu.VMEM((rows, cols), b16),
            pltpu.VMEM((2, half, rows, cols), b16),
            pltpu.VMEM((2, half, rows, cols), b16),
            pltpu.VMEM((2, half, rows, cols), b16),
            pltpu.VMEM((2, half, rows, cols), b16),
            pltpu.VMEM((2, 8, 128), f32),
            pltpu.VMEM((2, 8, 128), f32),
            pltpu.VMEM((2, 8, 128), f32),
            pltpu.VMEM((2, half, 8, 128), f32),
            dma((4,)),
            dma((2, 6)),
            dma((2, half)),
            dma((2, half)),
            dma((2, half)),
            dma((2, half)),
            dma((2, half)),
            dma((2, half)),
            dma((2, half)),
            dma((2, half)),
            dma((2,)),
            dma((2,)),
            dma((2, half)),
            dma((2, half)),
        ],
        compiler_params=pltpu.CompilerParams(
            collective_id=0, has_side_effects=True, vmem_limit_bytes=46000 * 1024
        ),
    )(
        tokens,
        states,
        norm_gain,
        query_weight,
        forget_weight,
        value_weight,
        gate_weight,
        output_weight,
        output_gain,
        bound_logits.reshape(1, cols),
    )
    return mixed, new


def solution(mesh):
    placed = (
        P("grp", "tp"),
        P(None, "grp", "tp", None, None),
        P(),
        P(None, None, "tp"),
        P(None, None, "tp"),
        P(None, None, "tp"),
        P(None, None, "tp"),
        P(None, "tp", None),
        P(None, "tp"),
        P("tp"),
    )
    return jax.shard_map(
        functools.partial(body, mesh.shape["tp"]),
        mesh=mesh,
        in_specs=placed,
        out_specs=(P("grp", "tp"), P(None, "grp", "tp", None, None)),
        check_vma=False,
    )
```
